512 devices in a mesh: sp: 32 (over z, x), tp: 16 (over y, core).
Axes of the slice: x: 4, y: 8, z: 8, core: 2. Of those that a mesh axis runs over, the one named last changes fastest.
Arguments:
- stream: bfloat16 [4096, 2048], P('sp'), may hold values from -15 to 15
- cotangent: bfloat16 [4096, 2048], P('sp'), may hold values from -6 to 6
- route_ids: int32 [4096, 2], P('sp'), may hold values from 0 to 31, all different within a row; in each aligned block of 128 rows (0 to 127, 128 to 255, ...) at most 16 rows name the same one
- route_weights: float32 [4096, 2], P('sp'), may hold values from 0.1 to 0.9
- w_gate: bfloat16 [32, 2048, 2048], P('sp', None, 'tp'), may hold values from -0.125 to 0.125
- w_up: bfloat16 [32, 2048, 2048], P('sp', None, 'tp'), may hold values from -0.125 to 0.125
- w_down: bfloat16 [32, 2048, 2048], P('sp', 'tp'), may hold values from -0.125 to 0.125
- out_proj: bfloat16 [2048, 512], P(None, 'tp'), may hold values from -0.25 to 0.25
- mixed: bfloat16 [512, 4096], P('tp', 'sp'), may hold values from -6 to 6
- rec_input: bfloat16 [512, 4096], P('tp', 'sp'), may hold values from -6 to 6
- branch_input: bfloat16 [512, 4096], P('tp', 'sp'), may hold values from -6 to 6
- state_before: float32 [512, 4096], P('tp', 'sp'), may hold values from -6 to 6
- rec_gates: bfloat16 [16, 32, 32], P('tp'), may hold values from -1 to 1
- in_gates: bfloat16 [16, 32, 32], P('tp'), may hold values from -1 to 1
- decay_param: float32 [512], P('tp'), may hold values from 4.4 to 11
- decay_shift: float32 [512, 4096], P('tp', 'sp'), may hold values from -1.4 to -1e-05
Outputs:
- grad_gate: bfloat16 [32, 2048, 2048], P('sp', None, 'tp')
- grad_up: bfloat16 [32, 2048, 2048], P('sp', None, 'tp')
- grad_down: bfloat16 [32, 2048, 2048], P('sp', 'tp')
- grad_proj: float32 [2048, 512], P('sp', 'tp')
- grad_rec: float32 [512, 4096], P('tp', 'sp')
- grad_branch: float32 [512, 4096], P('tp', 'sp')
The draws below stay inside these ranges and needn't reach their ends.
Inputs may be any that keep to these rules, and one draw needn't show every extreme that they name: `route_ids`: each row names 2 different experts; the rows of one device name no expert more than 16 times, a bound that some block reaches on some device.
All inputs are finite; a program needn't handle non-finite values.
Results may differ from the reference program's by a relative error of at most 0.03.
Values may be sent and summed in bfloat16 or wider, within the bound.
No kernel may reach another device: no remote copies, remote signals or barrier semaphores. Data moves between devices by JAX's collectives and lax.ppermute only.
A program may use at most 64 MiB of HBM per device.

```python
import math
import jax
import jax.numpy as jnp
import numpy as np
from jax import lax

D = 2048
F = 2048
W = 512
HD = 32
TOP_K = 2
TOK_DEV = 128
HEADS = 16
EXPERTS = 32
SEQUENCE_TOKENS = 4096
CAP = 16
N_SP = 32
N_TP = 16


def draw_decay_param(key, part):
    pick_key, fast_key, slow_key = jax.random.split(jax.random.fold_in(key, 11), 3)
    slow_share = 0.5
    slow_mask = jax.random.uniform(pick_key, (W,), jnp.float32) < slow_share
    fast_value = jax.random.uniform(fast_key, (W,), jnp.float32, 4.4, 5.2)
    slow_value = jax.random.uniform(slow_key, (W,), jnp.float32, 10.0, 11.0)
    return jnp.where(slow_mask, slow_value, fast_value).astype(jnp.float32)


def draw_decay_shift(key, part):
    block_key, location_key, size_key = jax.random.split(jax.random.fold_in(key, 23), 3)
    block_count = SEQUENCE_TOKENS // TOK_DEV
    block_rate = jax.random.uniform(block_key, (W, block_count), jnp.float32, 2e-05, 0.00015)
    stable_baseline = -jnp.repeat(block_rate, TOK_DEV, axis=1)
    spike_locations = jax.random.randint(location_key, (2,), 0, SEQUENCE_TOKENS)
    retained_fraction = jax.random.uniform(size_key, (2, W), jnp.float32, 0.5, 0.8)
    token_position = jnp.arange(SEQUENCE_TOKENS)
    match_count = token_position[None, None, :] == spike_locations[:, None, None]
    spike_events = jnp.sum(jnp.where(match_count, jnp.log(retained_fraction)[:, :, None], 0.0), axis=0)
    return (stable_baseline + spike_events).astype(jnp.float32)


def raised(entries, rng, source, target, parts, factor):
    def block_of(axis_at):
        return (jnp.arange(entries.shape[axis_at]) // (entries.shape[axis_at] // parts)).reshape((-1,) + (1,) * (entries.ndim - 1 - axis_at))

    first = jax.random.permutation(rng, parts)[block_of(target)]
    second = (block_of(target) + parts // 2) % parts
    return jnp.where((block_of(source) == first) | (block_of(source) == second), factor * entries, entries)


def shard_levels(rng, dims, cuts, low, largest):
    level, own = 1.0, jax.random.fold_in(rng, 6)
    for axis_at, blocks in cuts:
        heights = jnp.exp(jax.random.uniform(jax.random.fold_in(own, axis_at), (blocks,), jnp.float32, low / len(cuts), largest / len(cuts)))
        level = level * jnp.repeat(heights, dims[axis_at] // blocks).reshape([-1 if axis == axis_at else 1 for axis in range(len(dims))])
    return level


def shared_out(stream_key, own, number, rows, amount, top, limit, skew):
    order = jax.random.permutation(stream_key, amount)
    packed, ordinary = load_shares(amount, rows * top, limit, skew, True), load_shares(amount, rows * top, limit, skew, False)
    places = jnp.arange(amount)

    def named(tallies, turn):
        used = int((tallies > 0).sum())
        fixed = max(1, used // 4)
        passed = fixed + (places - fixed + turn * (used - fixed)) % max(1, amount - fixed)
        return jnp.zeros((amount,), jnp.int32).at[order[jnp.where(places < fixed, places, passed)]].set(jnp.asarray(tallies, jnp.int32))

    tallies = jnp.where(number % 4 == 0, named(packed, number // 4), named(ordinary, number - number // 4 - 1))
    mixed = jax.random.permutation(jax.random.fold_in(own, 3), amount)
    source_of, sink = mixed[0:amount // 2 * 2:2], mixed[1:amount // 2 * 2:2]
    room = jnp.minimum(tallies[source_of] - 1, limit - tallies[sink]) // 2
    room = jnp.where((source_of == order[0]) | (sink == order[0]) | (tallies[sink] == 0), 0, jnp.maximum(room, 0))
    passed = jax.random.randint(jax.random.fold_in(own, 4), (amount // 2,), 0, 1 << 20) % (room + 1)
    tallies = tallies.at[source_of].add(-passed).at[sink].add(passed)
    members = jnp.searchsorted(jnp.cumsum(tallies), jnp.arange(rows * top), side="right").astype(jnp.int32)
    grid = members.reshape(top, rows).T
    grid = grid[jax.random.permutation(jax.random.fold_in(own, 1), rows)]
    turn = jax.random.randint(jax.random.fold_in(own, 2), (rows, 1), 0, top)
    return jnp.take_along_axis(grid, (jnp.arange(top)[None, :] + turn) % top, axis=1)


def load_shares(amount, total, most, lean, full):
    portions = [(1 << 20) // math.isqrt(rank ** lean) + 1 for rank in range(1, amount + 1)]
    largest = most if full else min(most, max(-(-total // amount), total * portions[0] // sum(portions)))
    least = 1 if total - largest >= amount - 1 else 0
    counts, spare = [largest] + [least] * (amount - 1), total - largest - least * (amount - 1)
    while spare > 0:
        candidates = [i for i in range(1, amount) if counts[i] < largest] or [i for i in range(1, amount) if counts[i] < most]
        mass, budget = sum([portions[i] for i in candidates]), spare
        for i in candidates:
            addition = min(most - counts[i], max(1, budget * portions[i] // mass), spare)
            counts[i] = counts[i] + addition
            spare = spare - addition
    return np.array(counts)


def noise(key, extent, spread, bound, cuts=(), held_as=jnp.bfloat16):
    factor_of = shard_levels(key, extent, cuts, -0.22, 0.18) if cuts else 1.0
    drawn = jax.random.normal(key, extent, jnp.float32) * spread * factor_of
    return jnp.minimum(jnp.maximum(drawn, -bound), bound).astype(held_as)


def noise_with(own_key, shape, width, most, cuts, heavy, kind=jnp.bfloat16):
    array = width * jax.random.normal(own_key, shape, jnp.float32)
    if cuts:
        array = array * shard_levels(own_key, shape, cuts, -0.22, 0.18)
    return jnp.clip(raised(array, jax.random.fold_in(own_key, 3), *heavy), -most, most).astype(kind)


def setup_inputs(seed: int = 0) -> dict:
    arg_keys = jax.random.split(jax.random.key(seed), 17)
    stream = noise(arg_keys[0], (SEQUENCE_TOKENS, D), 2.5, 15.0, ((0, 32),))
    cotangent = noise_with(arg_keys[1], (SEQUENCE_TOKENS, D), 1.0, 6.0, ((0, 32),), (0, 1, 32, 2.75))
    route_ids_keys = jax.random.split(jax.random.fold_in(arg_keys[2], 1), SEQUENCE_TOKENS // TOK_DEV)
    route_ids_turns = jax.random.permutation(jax.random.fold_in(arg_keys[2], 3), SEQUENCE_TOKENS // TOK_DEV)
    route_ids = jax.vmap(lambda own, number: shared_out(jax.random.fold_in(arg_keys[2], 2), own, number, TOK_DEV, EXPERTS, TOP_K, CAP, 1))(route_ids_keys, route_ids_turns).reshape((SEQUENCE_TOKENS, TOP_K))
    route_weights = jnp.clip(0.1 + 0.79999997 * jax.random.uniform(arg_keys[3], (SEQUENCE_TOKENS, TOP_K), jnp.float32) ** shard_levels(arg_keys[3], (SEQUENCE_TOKENS, TOP_K), ((0, 32),), -0.2, 0.2), 0.1, 0.9)
    w_gate = noise(arg_keys[4], (EXPERTS, D, F), D ** -0.5, 0.125, ((0, 32), (2, 16)))
    w_up = noise(arg_keys[5], (EXPERTS, D, F), D ** -0.5, 0.125, ((0, 32), (2, 16)))
    w_down = noise(arg_keys[6], (EXPERTS, F, D), F ** -0.5, 0.125, ((0, 32), (1, 16)))
    out_proj = noise(arg_keys[7], (D, W), W ** -0.5, 0.25, ((1, 16),))
    mixed = noise(arg_keys[8], (W, SEQUENCE_TOKENS), 1.0, 6.0, ((0, 16), (1, 32)))
    rec_input = noise(arg_keys[9], (W, SEQUENCE_TOKENS), 1.0, 6.0, ((0, 16), (1, 32)))
    branch_input = noise(arg_keys[10], (W, SEQUENCE_TOKENS), 1.0, 6.0, ((0, 16), (1, 32)))
    state_before = noise(arg_keys[11], (W, SEQUENCE_TOKENS), 1.0, 6.0, ((0, 16), (1, 32)), jnp.float32)
    rec_gates = noise(arg_keys[12], (HEADS, HD, HD), HD ** -0.5, 1.0, ((0, 16),))
    in_gates = noise(arg_keys[13], (HEADS, HD, HD), HD ** -0.5, 1.0, ((0, 16),))
    decay_param = draw_decay_param(jax.random.fold_in(arg_keys[16], 71), 0)
    decay_shift = draw_decay_shift(jax.random.fold_in(arg_keys[16], 71), 0)
    return {"stream": stream, "cotangent": cotangent, "route_ids": route_ids, "route_weights": route_weights, "w_gate": w_gate, "w_up": w_up, "w_down": w_down, "out_proj": out_proj, "mixed": mixed, "rec_input": rec_input, "branch_input": branch_input, "state_before": state_before, "rec_gates": rec_gates, "in_gates": in_gates, "decay_param": decay_param, "decay_shift": decay_shift}


RATE_SCALE = 8.0
CLAMP_LIMIT = 7.0
GLU_ALPHA = 1.702

def expert_act(gate_pre, up_pre):
    glu_part = jnp.minimum(gate_pre, CLAMP_LIMIT)
    lin_part = jnp.clip(up_pre, -CLAMP_LIMIT, CLAMP_LIMIT)
    return glu_part * jax.nn.sigmoid(GLU_ALPHA * glu_part) * (lin_part + 1.0)

def reverse_step(later_elem, earlier_elem):
    return (later_elem[0] * earlier_elem[0], earlier_elem[1] + earlier_elem[0] * later_elem[1])

def reference(stream, cotangent, route_ids, route_weights, w_gate, w_up, w_down, out_proj, mixed, rec_input, branch_input, state_before, rec_gates, in_gates, decay_param, decay_shift):
    token_count, model_width = cotangent.shape
    top_count = route_ids.shape[1]
    expert_count = w_gate.shape[0]
    hidden = w_gate.shape[2]
    per_device = token_count // N_SP
    capacity = 2 * per_device * top_count // expert_count
    expert_rows = N_SP * capacity
    grouped = route_ids.reshape(N_SP, per_device * top_count)
    onehot = (grouped[:, :, None] == jnp.arange(expert_count, dtype=jnp.int32)[None, None, :]).astype(jnp.int32)
    slot_index = lax.optimization_barrier(jnp.sum((jnp.cumsum(onehot, axis=1) - onehot) * onehot, axis=2))
    device_ids = jnp.arange(N_SP, dtype=jnp.int32)[:, None]
    target = (grouped * expert_rows + device_ids * capacity + slot_index).reshape(-1).astype(jnp.int32)
    scaled = (route_weights[:, :, None] * cotangent[:, None, :].astype(jnp.float32)).astype(jnp.bfloat16)
    scaled = scaled.reshape(-1, model_width)
    copies = jnp.broadcast_to(stream[:, None, :], (token_count, top_count, model_width)).reshape(-1, model_width)
    empty_rows = jnp.zeros((expert_count * expert_rows, model_width), jnp.bfloat16)
    grad_rows = empty_rows.at[target].set(scaled).reshape(expert_count, expert_rows, model_width)
    token_rows = empty_rows.at[target].set(copies).reshape(expert_count, expert_rows, model_width)
    group_width = hidden // N_TP

    def one_expert(expert_item):
        grads_one, tokens_one, gate_one, up_one, down_one = expert_item
        gate_pre = jnp.dot(tokens_one, gate_one, preferred_element_type=jnp.float32)
        up_pre = jnp.dot(tokens_one, up_one, preferred_element_type=jnp.float32)
        act_val, act_vjp = jax.vjp(expert_act, gate_pre, up_pre)
        act_low = act_val.astype(jnp.bfloat16)
        d_act = jnp.dot(grads_one, down_one.T, preferred_element_type=jnp.float32)
        d_gate, d_up = act_vjp(d_act)
        d_gate = d_gate.astype(jnp.bfloat16)
        d_up = d_up.astype(jnp.bfloat16)
        g_gate = jnp.dot(tokens_one.T, d_gate, preferred_element_type=jnp.float32).astype(jnp.bfloat16)
        g_up = jnp.dot(tokens_one.T, d_up, preferred_element_type=jnp.float32).astype(jnp.bfloat16)
        g_down = jnp.dot(act_low.T, grads_one, preferred_element_type=jnp.float32).astype(jnp.bfloat16)
        gate_terms = jnp.einsum('rjf,djf->jrd', d_gate.astype(jnp.float32).reshape(expert_rows, N_TP, group_width), gate_one.astype(jnp.float32).reshape(model_width, N_TP, group_width))
        up_terms = jnp.einsum('rjf,djf->jrd', d_up.astype(jnp.float32).reshape(expert_rows, N_TP, group_width), up_one.astype(jnp.float32).reshape(model_width, N_TP, group_width))
        rounded = lax.optimization_barrier((gate_terms + up_terms).astype(jnp.bfloat16))
        summed = lax.optimization_barrier(jnp.sum(rounded.astype(jnp.float32), axis=0)).astype(jnp.bfloat16)
        return (g_gate, g_up, g_down, summed)
    grad_gate, grad_up, grad_down, slot_grads = lax.map(one_expert, (grad_rows, token_rows, w_gate, w_up, w_down))
    per_pair = slot_grads.reshape(-1, model_width)[target].astype(jnp.float32).reshape(token_count, top_count, model_width)
    stream_low = (cotangent.astype(jnp.float32) + lax.optimization_barrier(jnp.sum(per_pair, axis=1))).astype(jnp.bfloat16)
    d_mixed = lax.dot_general(out_proj, stream_low, (((0,), (1,)), ((), ())), preferred_element_type=jnp.float32)
    grad_proj = lax.dot_general(stream_low, mixed, (((0,), (1,)), ((), ())), preferred_element_type=jnp.float32)
    channels, positions = rec_input.shape
    gate_heads = rec_gates.shape[0]
    head_dim = rec_gates.shape[1]
    rec_value = rec_input.astype(jnp.float32)
    rec_heads = rec_value.reshape(gate_heads, head_dim, positions)
    rec_pre = jnp.einsum('hij,hit->hjt', rec_gates.astype(jnp.float32), rec_heads).reshape(channels, positions)
    in_pre = jnp.einsum('hij,hit->hjt', in_gates.astype(jnp.float32), rec_heads).reshape(channels, positions)
    rec_gate = jax.nn.sigmoid(rec_pre)
    in_gate = jax.nn.sigmoid(in_pre)
    soft_plus = jax.nn.softplus(-decay_param)[:, None]
    log_decay = -RATE_SCALE * rec_gate * soft_plus + decay_shift
    decay_rate = jnp.exp(log_decay)
    at_start = (jnp.arange(positions) == 0)[None, :]
    raw_mult = jnp.sqrt(-jnp.expm1(2.0 * log_decay))
    multiplier = jnp.where(at_start, 1.0, raw_mult)
    state_now = decay_rate * state_before + multiplier * in_gate * rec_value
    gelu_val, gelu_vjp = jax.vjp(jax.nn.gelu, branch_input.astype(jnp.float32))
    grad_branch = gelu_vjp(d_mixed * state_now)[0]
    d_state = d_mixed * gelu_val
    next_decay = jnp.concatenate([decay_rate[:, 1:], jnp.zeros((channels, 1), jnp.float32)], axis=1)
    adjoint = lax.associative_scan(reverse_step, (next_decay, d_state), reverse=True, axis=1)[1]
    mult_term = adjoint * in_gate * rec_value * decay_rate * decay_rate / raw_mult
    d_log = adjoint * state_before * decay_rate - jnp.where(at_start, 0.0, mult_term)
    d_rec_pre = (d_log * -RATE_SCALE * soft_plus * rec_gate * (1.0 - rec_gate)).astype(jnp.bfloat16)
    d_in_pre = (adjoint * multiplier * rec_value * in_gate * (1.0 - in_gate)).astype(jnp.bfloat16)
    d_rec_pre, d_in_pre = lax.optimization_barrier((d_rec_pre, d_in_pre))
    back_rec = jnp.einsum('hij,hjt->hit', rec_gates.astype(jnp.float32), d_rec_pre.astype(jnp.float32).reshape(gate_heads, head_dim, positions))
    back_in = jnp.einsum('hij,hjt->hit', in_gates.astype(jnp.float32), d_in_pre.astype(jnp.float32).reshape(gate_heads, head_dim, positions))
    grad_rec = adjoint * multiplier * in_gate + (back_rec + back_in).reshape(channels, positions)
    return (grad_gate, grad_up, grad_down, grad_proj, grad_rec, grad_branch)
```

```python
import functools

import jax
import jax.numpy as jnp
from jax import lax
from jax.experimental import pallas as pl
from jax.experimental.pallas import tpu as pltpu
from jax.sharding import PartitionSpec as P

RATE_SCALE = 8.0
CLAMP_LIMIT = 7.0
GLU_ALPHA = 1.702
F32 = jnp.float32
BF16 = jnp.bfloat16
GROUP = 4
SUB = 4


def dot(a, b, ca=1, cb=0):
    return lax.dot_general(a, b, (((ca,), (cb,)), ((), ())), preferred_element_type=F32)


def call(body, out, *args, flops=0, scratch=(), specs=None):
    out = tuple(out) if isinstance(out, (list, tuple)) else out
    return pl.pallas_call(
        body,
        out_shape=out,
        in_specs=specs if specs else [pl.BlockSpec(memory_space=pltpu.VMEM)] * len(args),
        scratch_shapes=list(scratch),
        cost_estimate=pl.CostEstimate(flops=flops, bytes_accessed=1 << 20, transcendentals=0),
    )(*args)


def sds(shape, dtype):
    return jax.ShapeDtypeStruct(shape, dtype)


def iota(shape, dim):
    return lax.broadcasted_iota(jnp.int32, shape, dim)


def pack_body(g_ref, u_ref, d_ref, o_ref):
    o_ref[:, 0:128] = g_ref[...]
    o_ref[:, 128:256] = u_ref[...]
    for j in range(d_ref.shape[1] // 128):
        o_ref[128 * j : 128 * (j + 1), 256:384] = d_ref[:, 128 * j : 128 * (j + 1)].T


def pack(w_gate, w_up, w_down):
    return call(pack_body, sds((w_gate.shape[0], 384), BF16), w_gate, w_up, w_down, flops=1 << 20)


def route_body(ids_ref, w_ref, stream_ref, cot_ref, o_ref):
    tok = stream_ref.shape[0]
    rows = o_ref.shape[0]
    sub = lax.axis_index("tp") % GROUP
    line = iota((rows, tok), 0)
    expert = line // 8
    slot = line % SUB + sub * SUB
    is_grad = (line % 8) >= SUB

    def along_lanes(ref, k):
        one = jnp.broadcast_to(ref[:, k : k + 1], (tok, tok)).T
        return jnp.concatenate([one] * (rows // tok), axis=0)

    first = along_lanes(ids_ref, 0) == expert
    second = along_lanes(ids_ref, 1) == expert
    named = first | second
    before = dot(
        jnp.where(named, 1.0, 0.0).astype(BF16),
        jnp.where(iota((tok, tok), 0) < iota((tok, tok), 1), 1.0, 0.0).astype(BF16),
    )
    here = named & (before == slot.astype(F32))
    weight = jnp.where(first, along_lanes(w_ref, 0), along_lanes(w_ref, 1))
    weight = jnp.sum(jnp.where(here & is_grad, weight, 0.0), axis=1, keepdims=True)
    weight = jnp.where(is_grad[:, 0:1], weight, 1.0)
    pick_x = jnp.where(here & ~is_grad, 1.0, 0.0).astype(BF16)
    pick_g = jnp.where(here & is_grad, 1.0, 0.0).astype(BF16)
    for j in range(stream_ref.shape[1] // 512):
        cols = slice(512 * j, 512 * (j + 1))
        both = dot(pick_x, stream_ref[:, cols]) + dot(pick_g, cot_ref[:, cols])
        o_ref[:, cols] = (both * weight).astype(BF16)


def expert_body(r_ref, *refs):
    weights, (o_ref, z_ref, buf, acc, sems) = refs[:GROUP], refs[GROUP:]
    rows = r_ref.shape[0]
    copies = [pltpu.make_async_copy(weights[k], buf.at[k], sems.at[k]) for k in range(GROUP)]
    for copy in copies:
        copy.start()
    is_x = (iota((rows, 128), 0) % 8) < SUB
    half = rows // 2
    want = iota((half, rows), 0)
    pick = (want // SUB) * 8 + want % SUB == iota((half, rows), 1)
    pick = jnp.where(pick, 1.0, 0.0).astype(BF16)
    for k in range(GROUP):
        copies[k].wait()
        pre = dot(r_ref[...], buf[k])
        gate, up = pre[:, 0:128], pre[:, 128:256]
        d_act = pltpu.roll(pre[:, 256:384], rows - SUB, 0)
        glu = jnp.minimum(gate, CLAMP_LIMIT)
        lin = jnp.clip(up, -CLAMP_LIMIT, CLAMP_LIMIT) + 1.0
        sig = jax.nn.sigmoid(GLU_ALPHA * glu)
        swish = glu * sig
        act = swish * lin
        slope = lin * (sig + GLU_ALPHA * swish * (1.0 - sig))
        d_gate = jnp.where(is_x & (gate <= CLAMP_LIMIT), d_act * slope, 0.0)
        d_up = jnp.where(is_x & (jnp.abs(up) <= CLAMP_LIMIT), d_act * swish, 0.0)
        act = jnp.where(is_x, 0.0, pltpu.roll(act, SUB, 0))
        d_both = jnp.concatenate([d_gate, d_up], axis=1).astype(BF16)
        z_ref[k, :, 0:256] = d_both
        z_ref[k, :, 256:384] = act.astype(BF16)
        d_rows = dot(pick, d_both).astype(BF16)
        part = dot(d_rows, buf[k, :, 0:256], 1, 1)
        if k == 0:
            acc[...] = part
        elif k < GROUP - 1:
            acc[...] += part
        else:
            total = acc[...] + part
            for j in range(o_ref.shape[0]):
                o_ref[j] = total[:, 128 * j : 128 * (j + 1)].astype(BF16)


def grads_body(r_ref, z_ref, own_ref, other_ref):
    turned = r_ref[...].T
    for ref, at, k in ((other_ref, 0, 1), (other_ref, 1, 3), (own_ref, 0, 0), (own_ref, 1, 2)):
        ref[at] = dot(turned, z_ref[k]).astype(BF16)


def combine_body(ids_ref, recv_ref, own_ref, o_ref):
    tok = own_ref.shape[0]
    lanes = recv_ref.shape[0] // GROUP
    col = iota((tok, lanes), 1)
    per_sub = lanes // GROUP
    slot = (col // per_sub) * SUB + col % SUB
    expert = (col % per_sub) // SUB
    named = (ids_ref[:, 0:1] == expert) | (ids_ref[:, 1:2] == expert)
    before = dot(
        jnp.where(iota((tok, tok), 0) > iota((tok, tok), 1), 1.0, 0.0).astype(BF16),
        jnp.where(named, 1.0, 0.0).astype(BF16),
    )
    pick = jnp.where(named & (before == slot.astype(F32)), 1.0, 0.0).astype(BF16)
    total = own_ref[...].astype(F32)
    for k in range(GROUP):
        total = total + dot(pick, recv_ref[lanes * k : lanes * (k + 1)])
    o_ref[...] = total.astype(BF16)


def in_three(x):
    high = x.astype(BF16)
    rest = x - high.astype(F32)
    mid = rest.astype(BF16)
    return high, mid, (rest - mid.astype(F32)).astype(BF16)


def scan_body(s_ref, proj_ref, mixed_ref, fac_ref, pay_ref, gb_ref, adj_ref, tail_ref):
    ch, tok = mixed_ref.shape
    blocks = s_ref.shape[0]
    low = iota((16, 128), 1) < 64
    d_mixed = jnp.zeros((ch, tok), F32)
    for j in range(blocks):
        s = s_ref[j]
        d_mixed = d_mixed + dot(proj_ref[:, 128 * j : 128 * (j + 1)], s, 1, 1)
        g = dot(mixed_ref[...], s)
        a, b = g[0:16], g[16:32]
        pay_ref[2 * j, 0:16] = jnp.where(low, a, pltpu.roll(b, 64, 1)).astype(BF16)
        pay_ref[2 * j + 1, 0:16] = jnp.where(low, pltpu.roll(a, 64, 1), b).astype(BF16)
    decay = fac_ref[0]
    gb_ref[...] = d_mixed * fac_ref[2]
    at = iota((ch, tok), 1)
    val = d_mixed * fac_ref[1]
    mul = jnp.where(at < tok - 1, pltpu.roll(decay, tok - 1, 1), 1.0)
    step = 1
    while step < tok:
        inside = at < tok - step
        later_val = jnp.where(inside, pltpu.roll(val, tok - step, 1), 0.0)
        later_mul = jnp.where(inside, pltpu.roll(mul, tok - step, 1), 1.0)
        val = val + mul * later_val
        mul = mul * later_mul
        step *= 2
    adj_ref[...] = val
    tail_ref[...] = mul
    first = at == 0
    head = jnp.sum(jnp.where(first, decay * val, 0.0), axis=1, keepdims=True)
    prod = jnp.sum(jnp.where(first, decay * mul, 0.0), axis=1, keepdims=True)
    cols = jnp.where(first, prod, jnp.where(at == 1, head, 0.0))
    cols = jnp.concatenate([cols, jnp.zeros((tok - ch, tok), F32)], axis=0)
    lines = cols.T[0:8]
    high, mid, rest = in_three(lines)
    lines = (
        high.astype(F32)
        + pltpu.roll(mid.astype(F32), 32, 1)
        + pltpu.roll(rest.astype(F32), 64, 1)
    ).astype(BF16)
    for k in range(pay_ref.shape[0]):
        pay_ref[k, 16:24] = lines


def finish_body(recv_ref, adj_ref, tail_ref, fac_ref, rg_ref, ig_ref, gp_ref, gr_ref):
    count = recv_ref.shape[0]
    me = lax.axis_index("sp")
    total = recv_ref[0, 0:16].astype(F32)
    for k in range(1, count):
        total = total + recv_ref[k, 0:16].astype(F32)
    turned = total.T
    gp_ref[:, 0:16] = turned[0:64]
    gp_ref[:, 16:32] = turned[64:128]
    carried = jnp.zeros((1, 128), F32)
    for k in range(count - 1, -1, -1):
        x = recv_ref[k, 16:24].astype(F32)
        x = x + pltpu.roll(x, 96, 1) + pltpu.roll(x, 64, 1)
        new = x[1:2] + x[0:1] * carried
        carried = jnp.where(k > me, new, carried)
    ch = adj_ref.shape[0]
    carried = jnp.broadcast_to(carried, (128, 128)).T[0:ch]
    adj = adj_ref[...] + tail_ref[...] * carried
    d_rec = (adj * fac_ref[3]).astype(BF16)
    d_in = (adj * fac_ref[4]).astype(BF16)
    gr_ref[...] = adj * fac_ref[5] + dot(rg_ref[...], d_rec) + dot(ig_ref[...], d_in)


def unpack_body(a_ref, b_ref, g_ref, u_ref, d_ref):
    for j in range(a_ref.shape[0] // 128):
        lines = slice(128 * j, 128 * (j + 1))
        total = a_ref[lines].astype(F32) + b_ref[lines].astype(F32)
        total = total.astype(BF16)
        g_ref[lines] = total[:, 0:128]
        u_ref[lines] = total[:, 128:256]
        d_ref[:, lines] = total[:, 256:384].T


def add_body(own_ref, got_ref, keep_ref, pass_ref):
    for ref, k in ((pass_ref, 1), (keep_ref, 0)):
        ref[...] = (own_ref[k].astype(F32) + got_ref[k].astype(F32)).astype(BF16)


def recurrence_factors(rec_input, branch_input, state_before, rec_gates, in_gates, decay_param, decay_shift):
    channels, positions = rec_input.shape
    rec_pre = dot(rec_gates, rec_input, 0, 0)
    in_pre = dot(in_gates, rec_input, 0, 0)
    rec_gate = jax.nn.sigmoid(rec_pre)
    in_gate = jax.nn.sigmoid(in_pre)
    soft_plus = jax.nn.softplus(-decay_param)[:, None]
    log_decay = -RATE_SCALE * rec_gate * soft_plus + decay_shift
    decay = jnp.exp(log_decay)
    at_start = (lax.axis_index("sp") * positions + jnp.arange(positions, dtype=jnp.int32) == 0)[None, :]
    raw_mult = jnp.sqrt(-jnp.expm1(2.0 * log_decay))
    multiplier = jnp.where(at_start, 1.0, raw_mult)
    rec_value = rec_input.astype(F32)
    state_now = decay * state_before + multiplier * in_gate * rec_value
    gelu_val, gelu_vjp = jax.vjp(jax.nn.gelu, branch_input.astype(F32))
    branch = gelu_vjp(state_now)[0]
    mult_term = jnp.where(at_start, 0.0, in_gate * rec_value * decay * decay / raw_mult)
    d_log = state_before * decay - mult_term
    d_rec = d_log * (-RATE_SCALE * soft_plus) * rec_gate * (1.0 - rec_gate)
    d_in = multiplier * rec_value * in_gate * (1.0 - in_gate)
    return jnp.stack([decay, gelu_val, branch, d_rec, d_in, multiplier * in_gate])


def local(
    stream,
    cotangent,
    route_ids,
    route_weights,
    w_gate,
    w_up,
    w_down,
    out_proj,
    mixed,
    rec_input,
    branch_input,
    state_before,
    rec_gates,
    in_gates,
    decay_param,
    decay_shift,
):
    sp_count, tp_count = lax.axis_size("sp"), lax.axis_size("tp")
    tok, width = cotangent.shape
    core = [(i, i ^ 1) for i in range(tp_count)]
    chip = [(i, i ^ 2) for i in range(tp_count)]

    own = pack(w_gate[0], w_up[0], w_down[0])
    across = lax.ppermute(own, "tp", chip)
    beside = lax.ppermute(own, "tp", core)
    rows = call(
        route_body,
        sds((sp_count * 8, width), BF16),
        route_ids,
        route_weights,
        stream,
        cotangent,
        flops=1 << 28,
    )
    recv = lax.all_to_all(rows.reshape(sp_count, 8, width), "sp", 0, 0, tiled=True)
    recv = recv.reshape(sp_count * 8, width)
    across_beside = lax.ppermute(across, "tp", core)
    vmem, hbm = pl.BlockSpec(memory_space=pltpu.VMEM), pl.BlockSpec(memory_space=pl.ANY)
    slots = sp_count * SUB
    terms, kept = call(
        expert_body,
        (sds((tp_count, slots, 128), BF16), sds((GROUP, sp_count * 8, 384), BF16)),
        recv,
        own,
        beside,
        across,
        across_beside,
        flops=1 << 31,
        specs=[vmem] + [hbm] * GROUP,
        scratch=(
            pltpu.VMEM((GROUP, width, 384), BF16),
            pltpu.VMEM((slots, width), F32),
            pltpu.SemaphoreType.DMA((GROUP,)),
        ),
    )
    back = lax.all_to_all(
        terms.reshape(tp_count * sp_count, SUB, 128), ("tp", "sp"), 0, 0, tiled=True
    ).reshape(-1, 128)
    grads_own, grads_other = call(
        grads_body,
        (sds((2, width, 384), BF16), sds((2, width, 384), BF16)),
        recv,
        kept,
        flops=1 << 31,
    )
    got = lax.ppermute(grads_other, "tp", core)
    keep, send = call(
        add_body, (sds((width, 384), BF16), sds((width, 384), BF16)), grads_own, got, flops=1 << 27
    )
    arrived = lax.ppermute(send, "tp", chip)

    own_cols = lax.dynamic_slice_in_dim(cotangent, lax.axis_index("tp") * 128, 128, 1)
    share = call(combine_body, sds((tok, 128), BF16), route_ids, back, own_cols, flops=1 << 27)
    low = lax.all_gather(share, "tp", axis=0)
    factors = recurrence_factors(
        rec_input, branch_input, state_before, rec_gates[0], in_gates[0], decay_param, decay_shift
    )
    channels = mixed.shape[0]
    plane = sds((channels, tok), F32)
    payload, grad_branch, adj, tail = call(
        scan_body,
        (sds((sp_count, 24, 128), BF16), plane, plane, plane),
        low,
        out_proj.T,
        mixed,
        factors,
        flops=1 << 27,
    )
    final = lax.all_to_all(payload, "sp", 0, 0, tiled=True)
    grad_proj, grad_rec = call(
        finish_body,
        (sds((width // sp_count, channels), F32), plane),
        final,
        adj,
        tail,
        factors,
        rec_gates[0],
        in_gates[0],
        flops=1 << 25,
    )
    grad_gate, grad_up, grad_down = call(
        unpack_body,
        (sds((width, 128), BF16), sds((width, 128), BF16), sds((128, width), BF16)),
        keep,
        arrived,
        flops=1 << 27,
    )
    return (grad_gate[None], grad_up[None], grad_down[None], grad_proj, grad_rec, grad_branch)


def solution(mesh):
    placed = (
        P("sp", None),
        P("sp", None),
        P("sp", None),
        P("sp", None),
        P("sp", None, "tp"),
        P("sp", None, "tp"),
        P("sp", "tp", None),
        P(None, "tp"),
        P("tp", "sp"),
        P("tp", "sp"),
        P("tp", "sp"),
        P("tp", "sp"),
        P("tp", None, None),
        P("tp", None, None),
        P("tp"),
        P("tp", "sp"),
    )
    return jax.shard_map(
        local,
        mesh=mesh,
        in_specs=placed,
        out_specs=(
            P("sp", None, "tp"),
            P("sp", None, "tp"),
            P("sp", "tp", None),
            P("sp", "tp"),
            P("tp", "sp"),
            P("tp", "sp"),
        ),
        check_vma=False,
    )
```

```python
import jax
import jax.numpy as jnp
from jax import lax
from jax.experimental import pallas as pl
from jax.experimental.pallas import tpu as pltpu
from jax.sharding import PartitionSpec as P


RATE_SCALE = 8.0
CLAMP_LIMIT = 7.0
GLU_ALPHA = 1.702
F32 = jnp.float32
BF16 = jnp.bfloat16
SUB = 4
PAIR = 2 * SUB


def dot(a, b, ca=1, cb=0):
    return lax.dot_general(a, b, (((ca,), (cb,)), ((), ())), preferred_element_type=F32)


def call(body, out, *args, flops=0, scratch=(), specs=None, grant=20):
    out = tuple(out) if isinstance(out, (list, tuple)) else out
    return pl.pallas_call(
        body,
        out_shape=out,
        in_specs=specs if specs else [pl.BlockSpec(memory_space=pltpu.VMEM)] * len(args),
        scratch_shapes=list(scratch),
        compiler_params=pltpu.CompilerParams(vmem_limit_bytes=grant << 20),
        cost_estimate=pl.CostEstimate(flops=flops, bytes_accessed=1 << 20, transcendentals=0),
    )(*args)


def sds(shape, dtype):
    return jax.ShapeDtypeStruct(shape, dtype)


def iota(shape, dim):
    return lax.broadcasted_iota(jnp.int32, shape, dim)


def route_body(ids_ref, w_ref, stream_ref, cot_ref, o_ref):
    tok, rows = stream_ref.shape[0], o_ref.shape[0]
    sub = lax.axis_index("y") % 2 * 2 + lax.axis_index("core")
    line = iota((rows, tok), 0)
    expert = line // 8
    slot = line % SUB + sub * SUB
    is_grad = (line % 8) >= SUB

    def along_lanes(ref, k):
        return jnp.broadcast_to(ref[k : k + 1, :], (rows, tok))

    first = along_lanes(ids_ref, 0) == expert
    second = along_lanes(ids_ref, 1) == expert
    named = first | second
    before = dot(
        jnp.where(named, 1.0, 0.0).astype(BF16),
        jnp.where(iota((tok, tok), 0) < iota((tok, tok), 1), 1.0, 0.0).astype(BF16),
    )
    here = named & (before == slot.astype(F32))
    weight = jnp.where(first, along_lanes(w_ref, 0), along_lanes(w_ref, 1))
    weight = jnp.sum(jnp.where(here & is_grad, weight, 0.0), axis=1, keepdims=True)
    weight = jnp.where(is_grad[:, 0:1], weight, 1.0)
    pick_x = jnp.where(here & ~is_grad, 1.0, 0.0).astype(BF16)
    pick_g = jnp.where(here & is_grad, 1.0, 0.0).astype(BF16)
    for j in range(stream_ref.shape[1] // 512):
        cols = slice(512 * j, 512 * (j + 1))
        both = dot(pick_x, stream_ref[:, cols]) + dot(pick_g, cot_ref[:, cols])
        o_ref[:, cols] = (both * weight).astype(BF16)


def expert_body(ra_ref, rb_ref, *refs):
    weights, (keep_ref, swap_ref, z_ref, both, down, rows_ref, sems) = refs[:6], refs[6:]
    part_rows = ra_ref.shape[0]
    rows = 2 * part_rows
    me = lax.axis_index("core")
    copies = []
    for k in range(2):
        places = (both.at[k, :, 0:128], both.at[k, :, 128:256], down.at[k])
        for n, place in enumerate(places):
            copies.append(pltpu.make_async_copy(weights[3 * k + n], place, sems.at[3 * k + n]))
    for copy in copies:
        copy.start()
    rows_ref[0:part_rows] = ra_ref[...]
    rows_ref[part_rows:rows] = rb_ref[...]
    is_x = (iota((rows, 128), 0) % 8) < SUB
    want = iota((part_rows, rows), 0)
    slot = want % PAIR
    source = jnp.where(slot // SUB == me, 0, part_rows) + (want // PAIR) * 8 + slot % SUB
    pick = jnp.where(source == iota((part_rows, rows), 1), 1.0, 0.0).astype(BF16)
    total = None
    for k in range(2):
        copies[3 * k].wait()
        copies[3 * k + 1].wait()
        pre = dot(rows_ref[...], both[k])
        copies[3 * k + 2].wait()
        d_act = pltpu.roll(dot(rows_ref[...], down[k], 1, 1), rows - SUB, 0)
        gate, up = pre[:, 0:128], pre[:, 128:256]
        glu = jnp.minimum(gate, CLAMP_LIMIT)
        lin = jnp.clip(up, -CLAMP_LIMIT, CLAMP_LIMIT) + 1.0
        sig = jax.nn.sigmoid(GLU_ALPHA * glu)
        swish = glu * sig
        act = swish * lin
        slope = lin * (sig + GLU_ALPHA * swish * (1.0 - sig))
        d_gate = jnp.where(is_x & (gate <= CLAMP_LIMIT), d_act * slope, 0.0)
        d_up = jnp.where(is_x & (jnp.abs(up) <= CLAMP_LIMIT), d_act * swish, 0.0)
        act = jnp.where(is_x, 0.0, pltpu.roll(act, SUB, 0))
        d_both = jnp.concatenate([d_gate, d_up], axis=1).astype(BF16)
        z_ref[k, :, 0:256] = d_both
        z_ref[k, :, 256:384] = act.astype(BF16)
        part = dot(dot(pick, d_both).astype(BF16), both[k], 1, 1)
        total = part if total is None else total + part
    for j in range(keep_ref.shape[0]):
        even = total[:, 256 * j : 256 * j + 128].astype(BF16)
        odd = total[:, 256 * j + 128 : 256 * j + 256].astype(BF16)
        keep_ref[j] = jnp.where(me == 0, even, odd)
        swap_ref[j] = jnp.where(me == 0, odd, even)


def grads_of(ra_ref, rb_ref, z_ref, k):
    rows = ra_ref.shape[0]
    return dot(ra_ref[...].T, z_ref[k, 0:rows]) + dot(rb_ref[...].T, z_ref[k, rows : 2 * rows])


def send_body(ra_ref, rb_ref, z_ref, o_ref):
    o_ref[...] = grads_of(ra_ref, rb_ref, z_ref, 1).astype(BF16)


def keep_body(ra_ref, rb_ref, z_ref, got_ref, gate_ref, up_ref, down_ref):
    total = grads_of(ra_ref, rb_ref, z_ref, 0) + got_ref[...].astype(F32)
    gate_ref[...] = total[:, 0:128].astype(BF16)
    up_ref[...] = total[:, 128:256].astype(BF16)
    for j in range(down_ref.shape[1] // 128):
        lines = slice(128 * j, 128 * (j + 1))
        down_ref[:, lines] = total[lines, 256:384].T.astype(BF16)


def places_body(ids_ref, o_ref):
    tok, lanes = o_ref.shape
    col = iota((tok, lanes), 1)
    half = lanes // 2
    slot = (col // half) * PAIR + col % PAIR
    expert = (col % half) // PAIR

    def named_by(k):
        one = jnp.broadcast_to(ids_ref[k : k + 1, :], (tok, tok)).T
        return jnp.concatenate([one] * (lanes // tok), axis=1) == expert

    named = named_by(0) | named_by(1)
    before = dot(
        jnp.where(iota((tok, tok), 0) > iota((tok, tok), 1), 1.0, 0.0).astype(BF16),
        jnp.where(named, 1.0, 0.0).astype(BF16),
    )
    o_ref[...] = jnp.where(named & (before == slot.astype(F32)), 1.0, 0.0).astype(BF16)


def combine_body(pick_ref, recv_ref, own_ref, o_ref):
    lanes = pick_ref.shape[1]
    total = own_ref[...].astype(F32)
    for k in range(recv_ref.shape[0] // lanes):
        total = total + dot(pick_ref[...], recv_ref[lanes * k : lanes * (k + 1)])
    o_ref[...] = total.astype(BF16)


def in_three(x):
    high = x.astype(BF16)
    rest = x - high.astype(F32)
    mid = rest.astype(BF16)
    return high, mid, (rest - mid.astype(F32)).astype(BF16)


def scan_body(s_ref, proj_ref, mixed_ref, fac_ref, pay_ref, gb_ref, adj_ref, tail_ref):
    ch, tok = mixed_ref.shape
    blocks = s_ref.shape[0]
    low = iota((16, 128), 1) < 64
    d_mixed = jnp.zeros((ch, tok), F32)
    for j in range(blocks):
        s = s_ref[j]
        d_mixed = d_mixed + dot(proj_ref[:, 128 * j : 128 * (j + 1)], s, 1, 1)
        g = dot(mixed_ref[...], s)
        a, b = g[0:16], g[16:32]
        pay_ref[2 * j, 0:16] = jnp.where(low, a, pltpu.roll(b, 64, 1)).astype(BF16)
        pay_ref[2 * j + 1, 0:16] = jnp.where(low, pltpu.roll(a, 64, 1), b).astype(BF16)
    decay = fac_ref[0]
    gb_ref[...] = d_mixed * fac_ref[2]
    at = iota((ch, tok), 1)
    val = d_mixed * fac_ref[1]
    mul = jnp.where(at < tok - 1, pltpu.roll(decay, tok - 1, 1), 1.0)
    step = 1
    while step < tok:
        inside = at < tok - step
        later_val = jnp.where(inside, pltpu.roll(val, tok - step, 1), 0.0)
        later_mul = jnp.where(inside, pltpu.roll(mul, tok - step, 1), 1.0)
        val = val + mul * later_val
        mul = mul * later_mul
        step *= 2
    adj_ref[...] = val
    tail_ref[...] = mul
    first = at == 0
    head = jnp.sum(jnp.where(first, decay * val, 0.0), axis=1, keepdims=True)
    prod = jnp.sum(jnp.where(first, decay * mul, 0.0), axis=1, keepdims=True)
    cols = jnp.where(first, prod, jnp.where(at == 1, head, 0.0))
    cols = jnp.concatenate([cols, jnp.zeros((tok - ch, tok), F32)], axis=0)
    lines = cols.T[0:8]
    high, mid, rest = in_three(lines)
    lines = (
        high.astype(F32)
        + pltpu.roll(mid.astype(F32), 32, 1)
        + pltpu.roll(rest.astype(F32), 64, 1)
    ).astype(BF16)
    for k in range(pay_ref.shape[0]):
        pay_ref[k, 16:24] = lines


def finish_body(recv_ref, adj_ref, tail_ref, fac_ref, rg_ref, ig_ref, gp_ref, gr_ref):
    count = recv_ref.shape[0]
    me = lax.axis_index("sp")
    total = recv_ref[0, 0:16].astype(F32)
    for k in range(1, count):
        total = total + recv_ref[k, 0:16].astype(F32)
    gp_ref[0:16] = total[:, 0:64]
    gp_ref[16:32] = total[:, 64:128]
    carried = jnp.zeros((1, 128), F32)
    for k in range(count - 1, -1, -1):
        x = recv_ref[k, 16:24].astype(F32)
        x = x + pltpu.roll(x, 96, 1) + pltpu.roll(x, 64, 1)
        new = x[1:2] + x[0:1] * carried
        carried = jnp.where(k > me, new, carried)
    ch = adj_ref.shape[0]
    carried = jnp.broadcast_to(carried, (128, 128)).T[0:ch]
    adj = adj_ref[...] + tail_ref[...] * carried
    d_rec = (adj * fac_ref[3]).astype(BF16)
    d_in = (adj * fac_ref[4]).astype(BF16)
    gr_ref[...] = adj * fac_ref[5] + dot(rg_ref[...], d_rec) + dot(ig_ref[...], d_in)


def recurrence_factors(rec_input, branch_input, state_before, rec_gates, in_gates, decay_param, decay_shift):
    _, positions = rec_input.shape
    rec_pre = dot(rec_gates, rec_input, 0, 0)
    in_pre = dot(in_gates, rec_input, 0, 0)
    rec_gate = jax.nn.sigmoid(rec_pre)
    in_gate = jax.nn.sigmoid(in_pre)
    soft_plus = jax.nn.softplus(-decay_param)[:, None]
    log_decay = -RATE_SCALE * rec_gate * soft_plus + decay_shift
    decay = jnp.exp(log_decay)
    at_start = (lax.axis_index("sp") * positions + jnp.arange(positions, dtype=jnp.int32) == 0)[None, :]
    raw_mult = jnp.sqrt(-jnp.expm1(2.0 * log_decay))
    multiplier = jnp.where(at_start, 1.0, raw_mult)
    rec_value = rec_input.astype(F32)
    state_now = decay * state_before + multiplier * in_gate * rec_value
    gelu_val, gelu_vjp = jax.vjp(jax.nn.gelu, branch_input.astype(F32))
    branch = gelu_vjp(state_now)[0]
    mult_term = jnp.where(at_start, 0.0, in_gate * rec_value * decay * decay / raw_mult)
    d_log = state_before * decay - mult_term
    d_rec = d_log * (-RATE_SCALE * soft_plus) * rec_gate * (1.0 - rec_gate)
    d_in = multiplier * rec_value * in_gate * (1.0 - in_gate)
    return jnp.stack([decay, gelu_val, branch, d_rec, d_in, multiplier * in_gate])


def local(
    stream,
    cotangent,
    route_ids,
    route_weights,
    w_gate,
    w_up,
    w_down,
    out_proj,
    mixed,
    rec_input,
    branch_input,
    state_before,
    rec_gates,
    in_gates,
    decay_param,
    decay_shift,
):
    sp_count, chips = lax.axis_size("sp"), lax.axis_size("y")
    tok, width = cotangent.shape
    core = [(0, 1), (1, 0)]
    chip = [(i, i ^ 1) for i in range(chips)]

    own = (w_gate[0], w_up[0], w_down[0])
    across = []
    for w in own:
        across.append(lax.ppermute(w, "y", chip))
    ids = route_ids.T
    lines = sp_count * PAIR
    rows = call(
        route_body,
        sds((lines, width), BF16),
        ids,
        route_weights.T,
        stream,
        cotangent,
        flops=1 << 28,
        grant=60,
    )
    mine = lax.all_to_all(rows.reshape(sp_count, 8, width), "sp", 0, 0, tiled=True)
    mine = mine.reshape(lines, width)
    theirs = lax.ppermute(mine, "core", core)
    vmem, hbm = pl.BlockSpec(memory_space=pltpu.VMEM), pl.BlockSpec(memory_space=pl.ANY)

    terms, terms_theirs, z = call(
        expert_body,
        (
            sds((chips, lines, 128), BF16),
            sds((chips, lines, 128), BF16),
            sds((2, 2 * lines, 384), BF16),
        ),
        mine,
        theirs,
        *own,
        *across,
        flops=1 << 31,
        specs=[vmem] * 2 + [hbm] * 6,
        scratch=(
            pltpu.VMEM((2, width, 256), BF16),
            pltpu.VMEM((2, 128, width), BF16),
            pltpu.VMEM((2 * lines, width), BF16),
            pltpu.SemaphoreType.DMA((6,)),
        ),
    )
    terms_got = lax.ppermute(terms_theirs, "core", core)
    grads = call(send_body, sds((width, 384), BF16), mine, theirs, z, flops=1 << 30)
    grads_got = lax.ppermute(grads, "y", chip)
    terms = (terms.astype(F32) + terms_got.astype(F32)).astype(BF16)
    terms = terms.reshape(chips * sp_count, PAIR, 128)
    back = lax.all_to_all(terms, ("y", "sp"), 0, 0, tiled=True)
    back = back.reshape(-1, 128)

    own_cols = lax.dynamic_slice_in_dim(cotangent, lax.axis_index(("y", "core")) * 128, 128, 1)
    pick = call(places_body, sds((tok, 2 * lines), BF16), ids, flops=1 << 25)
    share = call(combine_body, sds((tok, 128), BF16), pick, back, own_cols, flops=1 << 27)
    low = lax.all_gather(share, ("y", "core"), axis=0)
    factors = recurrence_factors(
        rec_input, branch_input, state_before, rec_gates[0], in_gates[0], decay_param, decay_shift
    )
    channels = mixed.shape[0]
    plane = sds((channels, tok), F32)
    payload, grad_branch, adj, tail = call(
        scan_body,
        (sds((sp_count, 24, 128), BF16), plane, plane, plane),
        low,
        out_proj.T,
        mixed,
        factors,
        flops=1 << 27,
    )
    final = lax.all_to_all(payload, "sp", 0, 0, tiled=True)
    grad_proj, grad_rec = call(
        finish_body,
        (sds((channels, width // sp_count), F32), plane),
        final,
        adj,
        tail,
        factors,
        rec_gates[0],
        in_gates[0],
        flops=1 << 25,
    )
    half = sds((width, 128), BF16)
    grad_gate, grad_up, grad_down = call(
        keep_body,
        (half, half, sds((128, width), BF16)),
        mine,
        theirs,
        z,
        grads_got,
        flops=1 << 30,
    )
    return (grad_gate[None], grad_up[None], grad_down[None], grad_proj.T, grad_rec, grad_branch)


def solution(mesh):
    devices = mesh.devices
    finer = jax.sharding.Mesh(
        devices.reshape(devices.shape[0], devices.shape[1] // 2, 2), ("sp", "y", "core")
    )
    placed = (
        P("sp", None),
        P("sp", None),
        P("sp", None),
        P("sp", None),
        P("sp", None, ("y", "core")),
        P("sp", None, ("y", "core")),
        P("sp", ("y", "core"), None),
        P(None, ("y", "core")),
        P(("y", "core"), "sp"),
        P(("y", "core"), "sp"),
        P(("y", "core"), "sp"),
        P(("y", "core"), "sp"),
        P(("y", "core"), None, None),
        P(("y", "core"), None, None),
        P(("y", "core")),
        P(("y", "core"), "sp"),
    )

    return jax.shard_map(
        local,
        mesh=finer,
        in_specs=placed,
        out_specs=(
            P("sp", None, ("y", "core")),
            P("sp", None, ("y", "core")),
            P("sp", ("y", "core"), None),
            P("sp", ("y", "core")),
            P(("y", "core"), "sp"),
            P(("y", "core"), "sp"),
        ),
        check_vma=False,
    )
```

```python
import jax
import jax.numpy as jnp
from jax import lax
from jax.experimental import pallas as pl
from jax.experimental.pallas import tpu as pltpu
from jax.sharding import PartitionSpec as P


RATE_SCALE = 8.0
CLAMP_LIMIT = 7.0
GLU_ALPHA = 1.702
F32 = jnp.float32
BF16 = jnp.bfloat16
SUB = 4
PAIR = 2 * SUB


def dot(a, b, ca=1, cb=0):
    return lax.dot_general(a, b, (((ca,), (cb,)), ((), ())), preferred_element_type=F32)


def call(body, out, *args, flops=0, scratch=(), specs=None, grant=20):
    out = tuple(out) if isinstance(out, (list, tuple)) else out
    return pl.pallas_call(
        body,
        out_shape=out,
        in_specs=specs if specs else [pl.BlockSpec(memory_space=pltpu.VMEM)] * len(args),
        scratch_shapes=list(scratch),
        compiler_params=pltpu.CompilerParams(vmem_limit_bytes=grant << 20),
        cost_estimate=pl.CostEstimate(flops=flops, bytes_accessed=1 << 20, transcendentals=0),
    )(*args)


def sds(shape, dtype):
    return jax.ShapeDtypeStruct(shape, dtype)


def iota(shape, dim):
    return lax.broadcasted_iota(jnp.int32, shape, dim)


def route_body(ids_ref, w_ref, stream_ref, cot_ref, o_ref):
    tok, rows = stream_ref.shape[0], o_ref.shape[0]
    sub = lax.axis_index("y") % 2 * 2 + lax.axis_index("core")
    line = iota((rows, tok), 0)
    expert = line // 8
    slot = line % SUB + sub * SUB
    is_grad = (line % 8) >= SUB

    def along_lanes(ref, k):
        return jnp.broadcast_to(ref[k : k + 1, :], (rows, tok))

    first = along_lanes(ids_ref, 0) == expert
    second = along_lanes(ids_ref, 1) == expert
    named = first | second
    before = dot(
        jnp.where(named, 1.0, 0.0).astype(BF16),
        jnp.where(iota((tok, tok), 0) < iota((tok, tok), 1), 1.0, 0.0).astype(BF16),
    )
    here = named & (before == slot.astype(F32))
    weight = jnp.where(first, along_lanes(w_ref, 0), along_lanes(w_ref, 1))
    weight = jnp.sum(jnp.where(here & is_grad, weight, 0.0), axis=1, keepdims=True)
    weight = jnp.where(is_grad[:, 0:1], weight, 1.0)
    pick_x = jnp.where(here & ~is_grad, 1.0, 0.0).astype(BF16)
    pick_g = jnp.where(here & is_grad, 1.0, 0.0).astype(BF16)
    for j in range(stream_ref.shape[1] // 512):
        cols = slice(512 * j, 512 * (j + 1))
        both = dot(pick_x, stream_ref[:, cols]) + dot(pick_g, cot_ref[:, cols])
        o_ref[:, cols] = (both * weight).astype(BF16)


def expert_math(rows, both, down):
    count = rows.shape[0]
    is_x = (iota((count, 128), 0) % 8) < SUB
    pre = dot(rows, both)
    d_act = pltpu.roll(dot(rows, down, 1, 1), count - SUB, 0)
    gate, up = pre[:, 0:128], pre[:, 128:256]
    glu = jnp.minimum(gate, CLAMP_LIMIT)
    lin = jnp.clip(up, -CLAMP_LIMIT, CLAMP_LIMIT) + 1.0
    sig = jax.nn.sigmoid(GLU_ALPHA * glu)
    swish = glu * sig
    act = swish * lin
    slope = lin * (sig + GLU_ALPHA * swish * (1.0 - sig))
    d_gate = jnp.where(is_x & (gate <= CLAMP_LIMIT), d_act * slope, 0.0)
    d_up = jnp.where(is_x & (jnp.abs(up) <= CLAMP_LIMIT), d_act * swish, 0.0)
    act = jnp.where(is_x, 0.0, pltpu.roll(act, SUB, 0)).astype(BF16)
    return jnp.concatenate([d_gate, d_up], axis=1).astype(BF16), act


def fetch(weights, both, down, sems):
    copies = []
    for k in range(len(weights) // 3):
        places = (both.at[k, :, 0:128], both.at[k, :, 128:256], down.at[k])
        for n, place in enumerate(places):
            copies.append(pltpu.make_async_copy(weights[3 * k + n], place, sems.at[3 * k + n]))
    for copy in copies:
        copy.start()
    return copies


def expert_body(ra_ref, rb_ref, *refs):
    weights, (keep_ref, swap_ref, z_ref, both, down, sems) = refs[:6], refs[6:]
    rows = ra_ref.shape[0]
    me = lax.axis_index("core")
    copies = fetch(weights, both, down, sems)
    want = iota((rows, rows), 0)
    slot = want % PAIR
    source = (want // PAIR) * 8 + slot % SUB == iota((rows, rows), 1)
    total = None
    for k in range(2):
        for copy in copies[3 * k : 3 * k + 3]:
            copy.wait()
        moved = None
        for n, ref in enumerate((ra_ref, rb_ref)):
            d_both, act = expert_math(ref[...], both[k], down[k])
            if k == 0:
                z_ref[n, :, 0:256] = d_both
                z_ref[n, :, 256:384] = act
            own = slot // SUB == (me if n == 0 else 1 - me)
            part = dot(jnp.where(source & own, 1.0, 0.0).astype(BF16), d_both)
            moved = part if moved is None else moved + part
        part = dot(moved.astype(BF16), both[k], 1, 1)
        total = part if total is None else total + part
    for j in range(keep_ref.shape[0]):
        even = total[:, 256 * j : 256 * j + 128].astype(BF16)
        odd = total[:, 256 * j + 128 : 256 * j + 256].astype(BF16)
        keep_ref[j] = jnp.where(me == 0, even, odd)
        swap_ref[j] = jnp.where(me == 0, odd, even)


def grads_body(ra_ref, rb_ref, rc_ref, rd_ref, z_ref, *refs):
    weights, (gate_ref, up_ref, down_ref, both, down, sems) = refs[:3], refs[3:]
    copies = fetch(weights, both, down, sems)
    total = None
    for n, ref in enumerate((ra_ref, rb_ref)):
        part = dot(ref[...].T, z_ref[n])
        total = part if total is None else total + part
    for copy in copies:
        copy.wait()
    for ref in (rc_ref, rd_ref):
        rows = ref[...]
        z = jnp.concatenate(expert_math(rows, both[0], down[0]), axis=1)
        total = total + dot(rows.T, z)
    gate_ref[...] = total[:, 0:128].astype(BF16)
    up_ref[...] = total[:, 128:256].astype(BF16)
    for j in range(down_ref.shape[1] // 128):
        lines = slice(128 * j, 128 * (j + 1))
        down_ref[:, lines] = total[lines, 256:384].T.astype(BF16)


def places_body(ids_ref, o_ref):
    tok, lanes = o_ref.shape
    col = iota((tok, lanes), 1)
    half = lanes // 2
    slot = (col // half) * PAIR + col % PAIR
    expert = (col % half) // PAIR

    def named_by(k):
        one = jnp.broadcast_to(ids_ref[k : k + 1, :], (tok, tok)).T
        return jnp.concatenate([one] * (lanes // tok), axis=1) == expert

    named = named_by(0) | named_by(1)
    before = dot(
        jnp.where(iota((tok, tok), 0) > iota((tok, tok), 1), 1.0, 0.0).astype(BF16),
        jnp.where(named, 1.0, 0.0).astype(BF16),
    )
    o_ref[...] = jnp.where(named & (before == slot.astype(F32)), 1.0, 0.0).astype(BF16)


def combine_body(pick_ref, recv_ref, own_ref, o_ref):
    lanes = pick_ref.shape[1]
    total = own_ref[...].astype(F32)
    for k in range(recv_ref.shape[0] // lanes):
        total = total + dot(pick_ref[...], recv_ref[lanes * k : lanes * (k + 1)])
    o_ref[...] = total.astype(BF16)


def in_three(x):
    high = x.astype(BF16)
    rest = x - high.astype(F32)
    mid = rest.astype(BF16)
    return high, mid, (rest - mid.astype(F32)).astype(BF16)


def scan_body(s_ref, proj_ref, mixed_ref, fac_ref, pay_ref, gb_ref, adj_ref, tail_ref):
    ch, tok = mixed_ref.shape
    blocks = s_ref.shape[0]
    low = iota((16, 128), 1) < 64
    d_mixed = jnp.zeros((ch, tok), F32)
    for j in range(blocks):
        s = s_ref[j]
        d_mixed = d_mixed + dot(proj_ref[:, 128 * j : 128 * (j + 1)], s, 1, 1)
        g = dot(mixed_ref[...], s)
        a, b = g[0:16], g[16:32]
        pay_ref[2 * j, 0:16] = jnp.where(low, a, pltpu.roll(b, 64, 1)).astype(BF16)
        pay_ref[2 * j + 1, 0:16] = jnp.where(low, pltpu.roll(a, 64, 1), b).astype(BF16)
    decay = fac_ref[0]
    gb_ref[...] = d_mixed * fac_ref[2]
    at = iota((ch, tok), 1)
    val = d_mixed * fac_ref[1]
    mul = jnp.where(at < tok - 1, pltpu.roll(decay, tok - 1, 1), 1.0)
    step = 1
    while step < tok:
        inside = at < tok - step
        later_val = jnp.where(inside, pltpu.roll(val, tok - step, 1), 0.0)
        later_mul = jnp.where(inside, pltpu.roll(mul, tok - step, 1), 1.0)
        val = val + mul * later_val
        mul = mul * later_mul
        step *= 2
    adj_ref[...] = val
    tail_ref[...] = mul
    first = at == 0
    head = jnp.sum(jnp.where(first, decay * val, 0.0), axis=1, keepdims=True)
    prod = jnp.sum(jnp.where(first, decay * mul, 0.0), axis=1, keepdims=True)
    cols = jnp.where(first, prod, jnp.where(at == 1, head, 0.0))
    cols = jnp.concatenate([cols, jnp.zeros((tok - ch, tok), F32)], axis=0)
    lines = cols.T[0:8]
    high, mid, rest = in_three(lines)
    lines = (
        high.astype(F32)
        + pltpu.roll(mid.astype(F32), 32, 1)
        + pltpu.roll(rest.astype(F32), 64, 1)
    ).astype(BF16)
    for k in range(pay_ref.shape[0]):
        pay_ref[k, 16:24] = lines


def finish_body(recv_ref, adj_ref, tail_ref, fac_ref, rg_ref, ig_ref, gp_ref, gr_ref):
    count = recv_ref.shape[0]
    me = lax.axis_index("sp")
    total = recv_ref[0, 0:16].astype(F32)
    for k in range(1, count):
        total = total + recv_ref[k, 0:16].astype(F32)
    gp_ref[0:16] = total[:, 0:64]
    gp_ref[16:32] = total[:, 64:128]
    carried = jnp.zeros((1, 128), F32)
    for k in range(count - 1, -1, -1):
        x = recv_ref[k, 16:24].astype(F32)
        x = x + pltpu.roll(x, 96, 1) + pltpu.roll(x, 64, 1)
        new = x[1:2] + x[0:1] * carried
        carried = jnp.where(k > me, new, carried)
    ch = adj_ref.shape[0]
    carried = jnp.broadcast_to(carried, (128, 128)).T[0:ch]
    adj = adj_ref[...] + tail_ref[...] * carried
    d_rec = (adj * fac_ref[3]).astype(BF16)
    d_in = (adj * fac_ref[4]).astype(BF16)
    gr_ref[...] = adj * fac_ref[5] + dot(rg_ref[...], d_rec) + dot(ig_ref[...], d_in)


def recurrence_factors(rec_input, branch_input, state_before, rec_gates, in_gates, decay_param, decay_shift):
    _, positions = rec_input.shape
    rec_pre = dot(rec_gates, rec_input, 0, 0)
    in_pre = dot(in_gates, rec_input, 0, 0)
    rec_gate = jax.nn.sigmoid(rec_pre)
    in_gate = jax.nn.sigmoid(in_pre)
    soft_plus = jax.nn.softplus(-decay_param)[:, None]
    log_decay = -RATE_SCALE * rec_gate * soft_plus + decay_shift
    decay = jnp.exp(log_decay)
    at_start = (lax.axis_index("sp") * positions + jnp.arange(positions, dtype=jnp.int32) == 0)[None, :]
    raw_mult = jnp.sqrt(-jnp.expm1(2.0 * log_decay))
    multiplier = jnp.where(at_start, 1.0, raw_mult)
    rec_value = rec_input.astype(F32)
    state_now = decay * state_before + multiplier * in_gate * rec_value
    gelu_val, gelu_vjp = jax.vjp(jax.nn.gelu, branch_input.astype(F32))
    branch = gelu_vjp(state_now)[0]
    mult_term = jnp.where(at_start, 0.0, in_gate * rec_value * decay * decay / raw_mult)
    d_log = state_before * decay - mult_term
    d_rec = d_log * (-RATE_SCALE * soft_plus) * rec_gate * (1.0 - rec_gate)
    d_in = multiplier * rec_value * in_gate * (1.0 - in_gate)
    return jnp.stack([decay, gelu_val, branch, d_rec, d_in, multiplier * in_gate])


def local(
    stream,
    cotangent,
    route_ids,
    route_weights,
    w_gate,
    w_up,
    w_down,
    out_proj,
    mixed,
    rec_input,
    branch_input,
    state_before,
    rec_gates,
    in_gates,
    decay_param,
    decay_shift,
):
    sp_count, chips = lax.axis_size("sp"), lax.axis_size("y")
    tok, width = cotangent.shape
    core = [(0, 1), (1, 0)]
    chip = [(i, i ^ 1) for i in range(chips)]

    own = (w_gate[0], w_up[0], w_down[0])
    across = []
    for w in own:
        across.append(lax.ppermute(w, "y", chip))
    ids = route_ids.T
    lines = sp_count * PAIR
    rows = call(
        route_body,
        sds((lines, width), BF16),
        ids,
        route_weights.T,
        stream,
        cotangent,
        flops=1 << 28,
        grant=60,
    )
    mine = lax.all_to_all(rows.reshape(sp_count, 8, width), "sp", 0, 0, tiled=True)
    mine = mine.reshape(lines, width)
    theirs = lax.ppermute(mine, "core", core)
    across_mine = lax.ppermute(mine, "y", chip)
    across_theirs = lax.ppermute(across_mine, "core", core)
    vmem, hbm = pl.BlockSpec(memory_space=pltpu.VMEM), pl.BlockSpec(memory_space=pl.ANY)

    terms, terms_theirs, z = call(
        expert_body,
        (
            sds((chips, lines, 128), BF16),
            sds((chips, lines, 128), BF16),
            sds((2, lines, 384), BF16),
        ),
        mine,
        theirs,
        *own,
        *across,
        flops=1 << 31,
        specs=[vmem] * 2 + [hbm] * 6,
        scratch=(
            pltpu.VMEM((2, width, 256), BF16),
            pltpu.VMEM((2, 128, width), BF16),
            pltpu.SemaphoreType.DMA((6,)),
        ),
    )
    terms_got = lax.ppermute(terms_theirs, "core", core)
    terms = (terms.astype(F32) + terms_got.astype(F32)).astype(BF16)
    terms = terms.reshape(chips * sp_count, PAIR, 128)
    back = lax.all_to_all(terms, ("y", "sp"), 0, 0, tiled=True)
    back = back.reshape(-1, 128)

    own_cols = lax.dynamic_slice_in_dim(cotangent, lax.axis_index(("y", "core")) * 128, 128, 1)
    pick = call(places_body, sds((tok, 2 * lines), BF16), ids, flops=1 << 25)
    share = call(combine_body, sds((tok, 128), BF16), pick, back, own_cols, flops=1 << 27)
    low = lax.all_gather(share, ("y", "core"), axis=0)
    factors = recurrence_factors(
        rec_input, branch_input, state_before, rec_gates[0], in_gates[0], decay_param, decay_shift
    )
    channels = mixed.shape[0]
    plane = sds((channels, tok), F32)
    payload, grad_branch, adj, tail = call(
        scan_body,
        (sds((sp_count, 24, 128), BF16), plane, plane, plane),
        low,
        out_proj.T,
        mixed,
        factors,
        flops=1 << 27,
    )
    final = lax.all_to_all(payload, "sp", 0, 0, tiled=True)
    grad_proj, grad_rec = call(
        finish_body,
        (sds((channels, width // sp_count), F32), plane),
        final,
        adj,
        tail,
        factors,
        rec_gates[0],
        in_gates[0],
        flops=1 << 25,
    )
    half = sds((width, 128), BF16)
    grad_gate, grad_up, grad_down = call(
        grads_body,
        (half, half, sds((128, width), BF16)),
        mine,
        theirs,
        across_mine,
        across_theirs,
        z,
        *own,
        flops=1 << 31,
        specs=[vmem] * 5 + [hbm] * 3,
        scratch=(
            pltpu.VMEM((1, width, 256), BF16),
            pltpu.VMEM((1, 128, width), BF16),
            pltpu.SemaphoreType.DMA((3,)),
        ),
    )
    return (grad_gate[None], grad_up[None], grad_down[None], grad_proj.T, grad_rec, grad_branch)


def solution(mesh):
    devices = mesh.devices
    finer = jax.sharding.Mesh(
        devices.reshape(devices.shape[0], devices.shape[1] // 2, 2), ("sp", "y", "core")
    )
    placed = (
        P("sp", None),
        P("sp", None),
        P("sp", None),
        P("sp", None),
        P("sp", None, ("y", "core")),
        P("sp", None, ("y", "core")),
        P("sp", ("y", "core"), None),
        P(None, ("y", "core")),
        P(("y", "core"), "sp"),
        P(("y", "core"), "sp"),
        P(("y", "core"), "sp"),
        P(("y", "core"), "sp"),
        P(("y", "core"), None, None),
        P(("y", "core"), None, None),
        P(("y", "core")),
        P(("y", "core"), "sp"),
    )

    return jax.shard_map(
        local,
        mesh=finer,
        in_specs=placed,
        out_specs=(
            P("sp", None, ("y", "core")),
            P("sp", None, ("y", "core")),
            P("sp", ("y", "core"), None),
            P("sp", ("y", "core")),
            P(("y", "core"), "sp"),
            P(("y", "core"), "sp"),
        ),
        check_vma=False,
    )
```
